256 devices in a mesh: grp: 4 (over y, x), ep: 64 (over z, core).
Axes of the slice: x: 2, y: 2, z: 32, core: 2. Of those that a mesh axis runs over, the one named last changes fastest.
The devices are a block of a 4x8x32 slice.
Arguments:
- tokens: bfloat16 [8192, 2048], P(('grp', 'ep')), parts along dimension 0, may hold values from -6 to 6
- routing: int32 [8192, 4], P(('grp', 'ep')), parts along dimension 0, may hold values from 0 to 63, as said below
- gate_weights: float32 [8192, 4], P(('grp', 'ep')), parts along dimension 0, may hold values from 0.05 to 1
- pre_gain: float32 [2048], replicated, may hold values from 0.1 to 1.9
- w_gate: bfloat16 [64, 2048, 512], P('ep'), may hold values from -0.125 to 0.125
- w_up: bfloat16 [64, 2048, 512], P('ep'), may hold values from -0.125 to 0.125
- w_down: bfloat16 [64, 512, 2048], P('ep'), may hold values from -0.25 to 0.25
- post_gain: float32 [2048], replicated, may hold values from 0.1 to 1.9
Outputs:
- mixed_out: bfloat16 [8192, 2048], P(('grp', 'ep')), parts along dimension 0
The draws below stay inside these ranges and needn't reach their ends.
There are 4 independent parts, one for each index of `grp`. The reference program is written for one: setup_inputs(seed, part) draws one part's arguments, and reference() takes and returns one part's arrays. A program takes and returns all parts, laid end to end along the dimension named above; an argument that names none is the same for every part. Nothing has to cross between parts.
Inputs may be any that keep to these rules, and one draw needn't show every extreme that they name: `routing`: each row names 4 different experts of one group (experts g * 8 to g * 8 + 7). The rows of one device name any one expert at most 4 times, and some expert exactly 4 times.
All inputs are finite; a program needn't handle non-finite values.
Results may differ from the reference program's by a relative error of at most 0.0085.
Values may be sent and summed in bfloat16 or wider, within the bound.
A program may use at most 64 MiB of HBM per device.

```python
import math
import jax
import jax.numpy as jnp
from jax import lax

D = 2048
EXPERT_FF = 512
TOPK = 4
EXP_GROUP = 8
TOK_DEV = 32
EXPERTS = 64
SPECIALIST_SETS = 8
CAP = 4
TOKENS = 2048
N_EP = 64


def draw_routing(key, part):
    group_slots = 2 * CAP
    slot_count = SPECIALIST_SETS * group_slots
    sampler_seeds = jax.random.split(key, 5)
    affinity_increment = jax.random.permutation(sampler_seeds[0], SPECIALIST_SETS).astype(jnp.int32) * (1024 // SPECIALIST_SETS)
    mandated_cluster = jax.random.randint(sampler_seeds[1], (N_EP,), 0, SPECIALIST_SETS)
    affinity_jitter = jax.random.randint(sampler_seeds[2], (N_EP, slot_count), 0, 1024)
    slot_ids = jnp.arange(slot_count, dtype=jnp.int32)
    cluster_for_position = slot_ids // group_slots
    cluster_affinity = affinity_jitter + affinity_increment[cluster_for_position][None, :] + jnp.where(cluster_for_position[None, :] == mandated_cluster[:, None], 4096, 0)
    cluster_affinity = cluster_affinity * slot_count + slot_ids[None, :]
    chosen = lax.top_k(cluster_affinity, TOK_DEV)[1].astype(jnp.int32)
    shuffle = jax.random.randint(sampler_seeds[3], (N_EP, TOK_DEV), 0, 1 << 20) * TOK_DEV + jnp.arange(TOK_DEV, dtype=jnp.int32)[None, :]
    chosen = jnp.take_along_axis(chosen, jnp.argsort(shuffle, axis=1, stable=True), axis=1)
    group_of = chosen // group_slots
    rank_of = chosen % group_slots
    offsets = jax.random.randint(sampler_seeds[4], (N_EP, SPECIALIST_SETS), 0, EXP_GROUP)
    offset_of = jnp.take_along_axis(offsets, group_of, axis=1)
    within = (offset_of[..., None] + rank_of[..., None] * TOPK + jnp.arange(TOPK, dtype=jnp.int32)) % EXP_GROUP
    return (group_of[..., None] * EXP_GROUP + within).reshape(TOKENS, TOPK).astype(jnp.int32)


def levels(stream_key, shape, cuts, low, largest):
    factor_of, own = 1.0, jax.random.fold_in(stream_key, 6)
    for axis_at, shards_of in cuts:
        heights = jnp.exp(jax.random.uniform(jax.random.fold_in(own, axis_at), (shards_of,), jnp.float32, low / len(cuts), largest / len(cuts)))
        factor_of = factor_of * jnp.repeat(heights, shape[axis_at] // shards_of).reshape([-1 if axis == axis_at else 1 for axis in range(len(shape))])
    return factor_of


def centred(key, extent, spread, bound, shards=(), kind=jnp.bfloat16):
    result = jax.random.normal(key, extent, jnp.float32) * spread
    if len(shards) > 0:
        result = levels(key, extent, shards, -0.22, 0.18) * result
    return jnp.clip(result, min=-bound, max=bound).astype(kind)


def setup_inputs(seed: int = 0, part: int = 0) -> dict:
    streams_of = jax.random.split(jax.random.key(seed), 9)
    part_splits = jax.random.split(jax.random.fold_in(streams_of[8], part), 9)
    return {
        "tokens": centred(part_splits[0], (TOKENS, D), 1.0, 6.0, ((0, 64),)),
        "routing": draw_routing(jax.random.fold_in(jax.random.fold_in(streams_of[8], part), 71), part),
        "gate_weights": jnp.clip(jnp.exp(math.log(1.0) - 2.9957323 * jax.random.uniform(part_splits[2], (TOKENS, TOPK), jnp.float32) ** levels(part_splits[2], (TOKENS, TOPK), ((0, 64),), -0.2, 0.2)), 0.05, 1.0),
        "pre_gain": jnp.clip(1.0 + 0.18 * jax.random.normal(streams_of[3], (D,), jnp.float32), 0.1, 1.9),
        "w_gate": centred(streams_of[4], (EXPERTS, D, EXPERT_FF), D ** -0.5, 0.125, ((0, 64),)),
        "w_up": centred(streams_of[5], (EXPERTS, D, EXPERT_FF), D ** -0.5, 0.125, ((0, 64),)),
        "w_down": centred(streams_of[6], (EXPERTS, EXPERT_FF, D), EXPERT_FF ** -0.5, 0.25, ((0, 64),)),
        "post_gain": jnp.clip(1.0 + 0.18 * jax.random.normal(streams_of[7], (D,), jnp.float32), 0.1, 1.9),
    }


epsilon = 1e-06

def normalize(values, gain):
    floats = values.astype(jnp.float32)
    return floats * lax.rsqrt(lax.optimization_barrier(jnp.mean(floats * floats, axis=-1, keepdims=True)) + epsilon) * gain

def reference(tokens, routing, gate_weights, pre_gain, w_gate, w_up, w_down, post_gain):
    normed = normalize(tokens, pre_gain).astype(jnp.bfloat16)
    flat_expert = routing.reshape(-1).astype(jnp.int32)
    flat_token = jnp.repeat(jnp.arange(TOKENS, dtype=jnp.int32), TOPK)
    flat_weight = gate_weights.reshape(-1)
    order = jnp.argsort(flat_expert, stable=True)
    sorted_token = flat_token[order]
    sorted_weight = flat_weight[order]
    counts = lax.optimization_barrier(jnp.sum((flat_expert[None, :] == jnp.arange(EXPERTS, dtype=jnp.int32)[:, None]).astype(jnp.int32), axis=1))
    starts = (jnp.cumsum(counts) - counts).astype(jnp.int32)
    most = CAP * N_EP
    token_pad = jnp.concatenate([sorted_token, jnp.full((most,), TOKENS, jnp.int32)])
    weight_pad = jnp.concatenate([sorted_weight, jnp.zeros((most,), jnp.float32)])
    normed_pad = jnp.concatenate([normed, jnp.zeros((1, D), normed.dtype)], axis=0)

    def one_expert(carry, expert):
        begin = starts[expert].astype(jnp.int32)
        index_rows = lax.dynamic_slice(token_pad, (begin,), (most,))
        weight_rows = lax.dynamic_slice(weight_pad, (begin,), (most,))
        live = jnp.arange(most) < counts[expert]
        index_rows = jnp.where(live, index_rows, TOKENS).astype(jnp.int32)
        weight_rows = jnp.where(live, weight_rows, 0.0)
        rows = normed_pad[index_rows]
        gate = jnp.dot(rows, w_gate[expert], preferred_element_type=jnp.float32)
        upward = jnp.dot(rows, w_up[expert], preferred_element_type=jnp.float32)
        hidden = (jax.nn.silu(gate) * upward).astype(jnp.bfloat16)
        output = jnp.dot(hidden, w_down[expert], preferred_element_type=jnp.float32).astype(jnp.bfloat16)
        carry = carry.at[index_rows].add(output.astype(jnp.float32) * weight_rows[:, None])
        return (carry, None)
    start_sum = jnp.zeros((TOKENS + 1, D), jnp.float32)
    mixture = lax.scan(one_expert, start_sum, jnp.arange(EXPERTS, dtype=jnp.int32))[0][:TOKENS]
    return normalize(mixture, post_gain).astype(jnp.bfloat16)
```

```python
import jax
import jax.numpy as jnp
from jax import lax
from jax.sharding import Mesh
from jax.sharding import PartitionSpec as P

SET = 8
TAIL = 128
EP = ("set", "mem")
ALL = ("grp", "set", "mem")

epsilon = 1e-06


def normalize(values, gain):
    floats = values.astype(jnp.float32)
    return floats * lax.rsqrt(jnp.mean(floats * floats, axis=-1, keepdims=True) + epsilon) * gain


def body(tokens, routing, gate_weights, pre_gain, w_gate, w_up, w_down, post_gain):
    normed = normalize(tokens, pre_gain).astype(jnp.bfloat16)
    tok_rows, width = tokens.shape
    sets = lax.axis_size("set")
    slots = sets * SET
    own_set = routing[:, 0] // SET
    same = (own_set[:, None] == own_set[None, :]) & (
        jnp.arange(tok_rows)[:, None] > jnp.arange(tok_rows)[None, :]
    )
    slot = own_set * SET + jnp.sum(same.astype(jnp.int32), axis=1)
    place = slot[None, :] == jnp.arange(slots)[:, None]
    member = routing % SET
    weights = jnp.sum(
        jnp.where(member[:, :, None] == jnp.arange(SET), gate_weights[:, :, None], 0.0), axis=1
    )
    high = weights.astype(jnp.bfloat16)
    low = (weights - high.astype(jnp.float32)).astype(jnp.bfloat16)
    tail = jnp.concatenate([high, low, jnp.zeros((tok_rows, TAIL - 2 * SET), jnp.bfloat16)], axis=1)
    rows = jnp.concatenate([normed, tail], axis=1)
    outbox = jnp.dot(
        place.astype(jnp.bfloat16), rows, preferred_element_type=jnp.float32
    ).astype(jnp.bfloat16)
    entered = lax.all_to_all(outbox, EP, split_axis=0, concat_axis=0, tiled=True)
    shared = lax.all_gather(entered, "mem", axis=0, tiled=True)
    x = shared[:, :width]
    mine = (jnp.arange(SET) == lax.axis_index("mem")).astype(jnp.float32)
    weight = jnp.sum(
        (
            shared[:, width : width + SET].astype(jnp.float32)
            + shared[:, width + SET : width + 2 * SET].astype(jnp.float32)
        )
        * mine,
        axis=1,
        keepdims=True,
    )
    gate = jnp.dot(x, w_gate[0], preferred_element_type=jnp.float32)
    upward = jnp.dot(x, w_up[0], preferred_element_type=jnp.float32)
    hidden = (jax.nn.silu(gate) * upward).astype(jnp.bfloat16)
    out = jnp.dot(hidden, w_down[0], preferred_element_type=jnp.float32)
    part = (out.astype(jnp.bfloat16).astype(jnp.float32) * weight).astype(jnp.bfloat16)
    summed = lax.psum_scatter(part, "mem", scatter_dimension=0, tiled=True)
    home = lax.all_to_all(summed, EP, split_axis=0, concat_axis=0, tiled=True)
    mixture = jnp.dot(
        place.T.astype(jnp.bfloat16), home, preferred_element_type=jnp.float32
    )
    return normalize(mixture, post_gain).astype(jnp.bfloat16)


def solution(mesh):
    ep = mesh.shape["ep"]
    split = Mesh(mesh.devices.reshape(mesh.shape["grp"], ep // SET, SET), ALL)
    placed = (
        P(ALL, None),
        P(ALL, None),
        P(ALL, None),
        P(),
        P(EP, None, None),
        P(EP, None, None),
        P(EP, None, None),
        P(),
    )
    return jax.shard_map(
        body, mesh=split, in_specs=placed, out_specs=P(ALL, None), check_vma=False
    )
```
